32 devices in a mesh: grp: 2 (over y), fs: 4 (over z), tp: 4 (over x, core).
Axes of the slice: x: 2, y: 2, z: 4, core: 2. Of those that a mesh axis runs over, the one named last changes fastest.
Arguments:
- tokens: bfloat16 [3072, 2048], P(('grp', 'fs'), 'tp'), parts along dimension 0, may hold values from -6 to 6
- norm_gain: float32 [2048], P('fs'), may hold values from 0.1 to 1.9
- gate_weight: float32 [4, 2048, 1024], P(None, 'fs', 'tp'), may hold values from -0.125 to 0.125
- up_weight: float32 [4, 2048, 1024], P(None, 'fs', 'tp'), may hold values from -0.125 to 0.125
- down_weight: float32 [4, 2048, 1024], P(None, 'fs', 'tp'), may hold values from -0.5 to 0.5
- expert_ids: int32 [3072, 2], P(('grp', 'fs')), parts along dimension 0, may hold values from 0 to 3, as said below
- group_logits: float32 [3072, 2], P(('grp', 'fs')), parts along dimension 0, may hold values from -2.5 to 2.5
- pair_logits: float32 [3072, 2], P(('grp', 'fs')), parts along dimension 0, may hold values from -2.5 to 2.5
Outputs:
- mixed: bfloat16 [3072, 2048], P(('grp', 'fs'), 'tp'), parts along dimension 0
- gate_out: bfloat16 [8, 2048, 1024], P(('grp', 'fs'), None, 'tp'), parts along dimension 0
- up_out: bfloat16 [8, 2048, 1024], P(('grp', 'fs'), None, 'tp'), parts along dimension 0
- down_out: bfloat16 [8, 2048, 1024], P(('grp', 'fs'), None, 'tp'), parts along dimension 0
The draws below stay inside these ranges and needn't reach their ends.
There are 2 independent parts, one for each index of `grp`. The reference program is written for one: setup_inputs(seed, part) draws one part's arguments, and reference() takes and returns one part's arrays. A program takes and returns all parts, laid end to end along the dimension named above; an argument that names none is the same for every part. Nothing has to cross between parts.
Inputs may be any that keep to these rules, and one draw needn't show every extreme that they name: `expert_ids`: each row names two different experts of one group: both ids lie in the same run of 2 consecutive ids.
All inputs are finite; a program needn't handle non-finite values.
Results may differ from the reference program's by a relative error of at most 0.015.
Values may be sent and summed in bfloat16 or wider, within the bound.
No kernel may reach another device: no remote copies, remote signals or barrier semaphores. Data moves between devices by JAX's collectives and lax.ppermute only.
A program may use at most 64 MiB of HBM per device.

```python
from functools import partial
import jax
import jax.numpy as jnp
from jax import lax

D = 2048
FF = 1024
GROUPS = 2
TOP = 2
TOK_DEV = 384
EXPERTS = 4
EXP_GROUP = 2
CAP = 240
TOKENS = 1536
N_FS = 4
N_TP = 4


def pick_by_weight(key, table):
    running = jnp.cumsum(table, axis=1)
    total = running[:, -1]
    draw = jax.random.randint(key, (table.shape[0],), 0, 1 << 30) % total
    return jnp.sum((running <= draw[:, None]).astype(jnp.int32), axis=1).astype(jnp.int32)


def draw_expert_ids(key, part):
    base = jax.random.fold_in(key, 11)
    key_hot, key_first, key_second = jax.random.split(base, 3)
    block_count = TOKENS // TOK_DEV
    block_keys = jax.random.split(key_hot, block_count)
    orders = jax.vmap(lambda single: jax.random.permutation(single, EXPERTS))(block_keys)
    block_table = 1 + 2 * (orders < EXPERTS // 2).astype(jnp.int32)
    token_block = jnp.arange(TOKENS, dtype=jnp.int32) // TOK_DEV
    token_table = block_table[token_block]
    first_pick = pick_by_weight(key_first, token_table)
    columns = jnp.arange(EXPERTS, dtype=jnp.int32)
    allowed = (columns[None, :] // EXP_GROUP == (first_pick // EXP_GROUP)[:, None]) & (columns[None, :] != first_pick[:, None])
    second_table = token_table * allowed.astype(jnp.int32)
    second_pick = pick_by_weight(key_second, second_table)
    return jnp.stack([first_pick, second_pick], axis=1).astype(jnp.int32)


def draw_tokens(key, part):
    base = jax.random.fold_in(key, 21)
    raw = jnp.clip(jax.random.normal(base, (TOKENS, D), jnp.float32), -3.0, 3.0)
    factor = 1.0 / jnp.sqrt(jnp.mean(raw * raw, axis=1, keepdims=True) + 1e-06)
    return jnp.clip(raw * factor, -6.0, 6.0).astype(jnp.bfloat16)


def draw_group_logits(key, part):
    base = jax.random.fold_in(key, 31)
    values = jnp.clip(0.6 * jax.random.normal(base, (TOKENS, GROUPS), jnp.float32), -2.5, 2.5)
    return values.astype(jnp.float32)


def draw_pair_logits(key, part):
    base = jax.random.fold_in(key, 41)
    values = jnp.clip(0.6 * jax.random.normal(base, (TOKENS, TOP), jnp.float32), -2.5, 2.5)
    return values.astype(jnp.float32)


def shard_levels(key, shape, cuts, low, high):
    def one(axis_at, blocks):
        steps = jax.random.uniform(jax.random.fold_in(jax.random.fold_in(key, 6), axis_at), (blocks,), jnp.float32, low / len(cuts), high / len(cuts))
        return jnp.repeat(jnp.exp(steps), shape[axis_at] // blocks).reshape((-1,) + (1,) * (len(shape) - axis_at - 1))

    level = one(*cuts[0])
    for cut in cuts[1:]:
        level = level * one(*cut)
    return level


def bell_draw(rng, extent, scale, most, cuts=(), kind=jnp.bfloat16):
    values = jax.random.normal(rng, extent, jnp.float32) * scale
    if len(cuts) > 0:
        values = shard_levels(rng, extent, cuts, -0.22, 0.18) * values
    return jnp.clip(values, min=-most, max=most).astype(kind)


def setup_inputs(seed: int = 0, part: int = 0) -> dict:
    key_of = jax.random.split(jax.random.key(seed), 9)
    own_keys = jax.random.split(jax.random.fold_in(key_of[8], part), 9)
    tokens = draw_tokens(jax.random.fold_in(jax.random.fold_in(key_of[8], part), 71), part)
    norm_gain = jnp.clip(1.0 + 0.18 * jax.random.normal(key_of[1], (D,), jnp.float32), 0.1, 1.9)
    gate_weight = bell_draw(key_of[2], (EXPERTS, D, FF), D ** -0.5, 0.125, ((1, 4), (2, 4)), jnp.float32)
    up_weight = bell_draw(key_of[3], (EXPERTS, D, FF), D ** -0.5, 0.125, ((1, 4), (2, 4)), jnp.float32)
    down_weight = bell_draw(key_of[4], (EXPERTS, D, FF), (FF // 8) ** -0.5, 0.5, ((1, 4), (2, 4)), jnp.float32)
    expert_ids = draw_expert_ids(jax.random.fold_in(jax.random.fold_in(key_of[8], part), 71), part)
    group_logits = draw_group_logits(jax.random.fold_in(jax.random.fold_in(key_of[8], part), 71), part)
    pair_logits = draw_pair_logits(jax.random.fold_in(jax.random.fold_in(key_of[8], part), 71), part)
    return dict(tokens=tokens, norm_gain=norm_gain, gate_weight=gate_weight, up_weight=up_weight, down_weight=down_weight, expert_ids=expert_ids, group_logits=group_logits, pair_logits=pair_logits)


def routing(block_ids, experts, capacity):
    entries = block_ids.reshape(-1).astype(jnp.int32)
    onehot = (entries[:, None] == jnp.arange(experts, dtype=jnp.int32)[None, :]).astype(jnp.int32)
    before = jnp.cumsum(onehot, axis=0) - onehot
    entry_rank = jnp.sum(before * onehot, axis=1)
    kept = entry_rank < capacity
    slot_index = jnp.where(kept, entries * capacity + entry_rank, experts * capacity)
    return slot_index.astype(jnp.int32), kept


def fill_slots(block_rows, slot_index, experts, capacity):
    entry_count = slot_index.shape[0]
    source_row = jnp.arange(entry_count, dtype=jnp.int32) // 2
    slot_row = jnp.zeros((experts * capacity + 1,), jnp.int32).at[slot_index].set(source_row)
    filled = jnp.zeros((experts * capacity + 1,), jnp.float32).at[slot_index].set(1.0)
    chosen = block_rows[slot_row[:experts * capacity]]
    return chosen * filled[:experts * capacity, None].astype(block_rows.dtype)


def route_weights(block_ids, group_logits, pair_logits, kept, exp_group):
    group_pick = block_ids[:, 0] // exp_group
    group_exp = jnp.exp(group_logits)
    columns = jnp.arange(group_logits.shape[1], dtype=jnp.int32)
    chosen = jnp.sum(jnp.where(columns[None, :] == group_pick[:, None], group_exp, 0.0), axis=1)
    chosen = chosen / jnp.sum(group_exp, axis=1)
    pair_exp = jnp.exp(pair_logits)
    weights = pair_exp / jnp.sum(pair_exp, axis=1, keepdims=True) * chosen[:, None]
    return weights * kept.reshape(-1, 2).astype(weights.dtype)


def expert_apply(operands):
    slot_rows, gate_matrix, up_matrix, down_matrix = operands
    gate = jnp.dot(slot_rows, gate_matrix, preferred_element_type=jnp.float32)
    up_part = jnp.dot(slot_rows, up_matrix, preferred_element_type=jnp.float32)
    hidden = (jax.nn.silu(gate) * up_part).astype(jnp.bfloat16)
    width = FF // N_TP
    total = jnp.zeros((slot_rows.shape[0], D), jnp.float32)
    for column in range(N_TP):
        term = lax.dot_general(hidden[:, column * width:(column + 1) * width],
                               down_matrix[:, column * width:(column + 1) * width],
                               (((1,), (1,)), ((), ())), preferred_element_type=jnp.float32)
        rounded = lax.optimization_barrier(term.astype(jnp.bfloat16))
        total = total + rounded.astype(jnp.float32)
    return total.astype(jnp.bfloat16)


def combine_block(returned, slot_index, weights):
    limit = returned.shape[0] - 1
    picked = returned[jnp.clip(slot_index, 0, limit)].astype(jnp.float32)
    picked = picked.reshape(weights.shape[0], 2, -1)
    return jnp.sum(picked * weights[:, :, None], axis=1).astype(jnp.bfloat16)


def reference(tokens, norm_gain, gate_weight, up_weight, down_weight, expert_ids, group_logits, pair_logits):
    scaled = norm_gain[None, :, None]
    gate_out = (scaled * gate_weight).astype(jnp.bfloat16)
    up_out = (scaled * up_weight).astype(jnp.bfloat16)
    down_out = down_weight.astype(jnp.bfloat16)
    id_blocks = expert_ids.reshape(N_FS, TOK_DEV, 2)
    token_blocks = tokens.reshape(N_FS, TOK_DEV, D)
    slot_index, kept = jax.vmap(partial(routing, experts=EXPERTS, capacity=CAP))(id_blocks)
    buffers = jax.vmap(partial(fill_slots, experts=EXPERTS, capacity=CAP))(token_blocks, slot_index)
    buffers = buffers.reshape(N_FS, EXPERTS, CAP, D).transpose(1, 0, 2, 3).reshape(EXPERTS, N_FS * CAP, D)
    results = lax.map(expert_apply, (buffers, gate_out, up_out, down_out))
    results = results.reshape(EXPERTS, N_FS, CAP, D).transpose(1, 0, 2, 3).reshape(N_FS, EXPERTS * CAP, D)
    weights = jax.vmap(partial(route_weights, exp_group=EXP_GROUP))(
        id_blocks, group_logits.reshape(N_FS, TOK_DEV, -1), pair_logits.reshape(N_FS, TOK_DEV, 2), kept)
    mixed = jax.vmap(combine_block)(results, slot_index, weights)
    return (mixed.reshape(TOKENS, D), gate_out, up_out, down_out)
```

```python
import jax
import jax.numpy as jnp
from jax import lax
from jax.experimental import pallas as pl
from jax.experimental.pallas import tpu as pltpu
from jax.sharding import PartitionSpec as P


def routing(block_ids, experts, capacity):
    entries = block_ids.reshape(-1)
    onehot = (entries[:, None] == jnp.arange(experts, dtype=jnp.int32)[None, :]).astype(jnp.int32)
    before = jnp.cumsum(onehot, axis=0) - onehot
    entry_rank = jnp.sum(before * onehot, axis=1)
    kept = entry_rank < capacity
    slot_index = jnp.where(kept, entries * capacity + entry_rank, experts * capacity)
    return (slot_index, kept)


def fill_slots(block_rows, slot_index, experts, capacity):
    entry_count = slot_index.shape[0]
    source_row = jnp.arange(entry_count, dtype=jnp.int32) // 2
    slot_row = jnp.zeros((experts * capacity + 1,), jnp.int32).at[slot_index].set(source_row)
    filled = jnp.zeros((experts * capacity + 1,), jnp.float32).at[slot_index].set(1.0)
    chosen = block_rows[slot_row[: experts * capacity]]
    return chosen * filled[: experts * capacity, None].astype(block_rows.dtype)


def route_weights(block_ids, group_logits, pair_logits, kept, exp_group):
    group_pick = block_ids[:, 0] // exp_group
    group_exp = jnp.exp(group_logits)
    columns = jnp.arange(group_logits.shape[1], dtype=jnp.int32)
    chosen = jnp.sum(jnp.where(columns[None, :] == group_pick[:, None], group_exp, 0.0), axis=1)
    chosen = chosen / jnp.sum(group_exp, axis=1)
    pair_exp = jnp.exp(pair_logits)
    weights = pair_exp / jnp.sum(pair_exp, axis=1, keepdims=True) * chosen[:, None]
    return weights * kept.reshape(-1, 2).astype(weights.dtype)


def general_body(
    tokens, norm_gain, gate_weight, up_weight, down_weight, expert_ids, group_logits, pair_logits
):
    experts = gate_weight.shape[0]
    tok_rows = tokens.shape[0]
    capacity = 5 * tok_rows * 2 // (4 * experts)
    shard_count = lax.axis_size("fs")
    scaled = norm_gain[None, :, None]
    gate_cast = (scaled * gate_weight).astype(jnp.bfloat16)
    up_cast = (scaled * up_weight).astype(jnp.bfloat16)
    down_cast = down_weight.astype(jnp.bfloat16)
    slot_index, kept = routing(expert_ids, experts, capacity)
    weights = route_weights(
        expert_ids, group_logits, pair_logits, kept, experts // group_logits.shape[1]
    )
    gate_here, up_here, down_here = (
        lax.all_to_all(gate_cast, "fs", split_axis=0, concat_axis=1, tiled=True),
        lax.all_to_all(up_cast, "fs", split_axis=0, concat_axis=1, tiled=True),
        lax.all_to_all(down_cast, "fs", split_axis=0, concat_axis=1, tiled=True),
    )
    gate_local = gate_here[0]
    up_local = up_here[0]
    outgoing = fill_slots(tokens, slot_index, experts, capacity)
    arrived = lax.all_to_all(
        outgoing.reshape(experts, capacity, -1), "fs", split_axis=0, concat_axis=0, tiled=True
    )
    arrived = arrived.reshape(shard_count * capacity, -1)
    piece = lax.all_gather(arrived, "tp", axis=1, tiled=True)
    gate_pre = jnp.dot(piece, gate_local, preferred_element_type=jnp.float32)
    up_pre = jnp.dot(piece, up_local, preferred_element_type=jnp.float32)
    hidden = (jax.nn.silu(gate_pre) * up_pre).astype(jnp.bfloat16)
    terms = lax.dot_general(
        hidden, down_here[0], (((1,), (1,)), ((), ())), preferred_element_type=jnp.float32
    )
    expert_rows = lax.psum_scatter(
        terms.astype(jnp.bfloat16), "tp", scatter_dimension=1, tiled=True
    )
    returned = lax.all_to_all(
        expert_rows.reshape(shard_count, capacity, -1),
        "fs",
        split_axis=0,
        concat_axis=0,
        tiled=True,
    )
    returned = returned.reshape(experts * capacity, -1)
    picked = returned[jnp.clip(slot_index, 0, experts * capacity - 1)].astype(jnp.float32)
    picked = picked.reshape(tok_rows, 2, -1)
    mixed = jnp.sum(picked * weights[:, :, None], axis=1).astype(jnp.bfloat16)
    return (mixed, gate_here, up_here, down_here)


VMEM = pl.BlockSpec(memory_space=pltpu.VMEM)
ANY = pl.BlockSpec(memory_space=pl.ANY)
F32 = jnp.float32
BF16 = jnp.bfloat16


def swap(value, axis, step):
    count = lax.axis_size(axis)
    return lax.ppermute(value, axis, [(i, i ^ step) for i in range(count)])


def aligned(start, size):
    return pl.ds(pl.multiple_of(start, size), size)


def as_column(row, lanes):
    return jnp.transpose(jnp.broadcast_to(row, (lanes, row.shape[1])))


def group_ranks(ids, exp_group):
    n = ids.shape[1]
    group = lax.div(ids[0:1, :], jnp.full((1, n), exp_group, jnp.int32))
    first = group == 0
    earlier = (
        lax.broadcasted_iota(jnp.int32, (n, n), 0) < lax.broadcasted_iota(jnp.int32, (n, n), 1)
    )
    ones = jnp.broadcast_to(jnp.where(first, 1.0, 0.0), (16, n)).astype(BF16)
    before = jnp.dot(
        ones, jnp.where(earlier, 1.0, 0.0).astype(BF16), preferred_element_type=F32
    )[0:1, :]
    place = lax.broadcasted_iota(jnp.int32, (1, n), 1)
    before = before.astype(jnp.int32)
    return group, jnp.where(first, before, place - before)


def gather_rows(ids_t, tokens, capacity, exp_group):
    def kernel(ids_ref, tok_ref, own_ref, other_ref):
        group, rank = group_ranks(ids_ref[...], exp_group)
        mine = lax.div(lax.axis_index("fs"), exp_group)
        n = tok_ref.shape[0]
        hit = lax.broadcasted_iota(jnp.int32, (capacity, n), 0) == rank
        tok = tok_ref[...]
        for out_ref, wanted in ((own_ref, mine), (other_ref, 1 - mine)):
            pick = jnp.where(hit & (group == wanted), 1.0, 0.0).astype(BF16)
            out_ref[...] = jnp.dot(pick, tok, preferred_element_type=F32).astype(BF16)

    shape = jax.ShapeDtypeStruct((capacity, tokens.shape[1]), BF16)
    return pl.pallas_call(
        kernel, out_shape=(shape, shape), in_specs=[VMEM, VMEM], out_specs=(VMEM, VMEM),
        name="gather_rows",
    )(ids_t, tokens)


def cast_pieces(gain, weights, steps, scaled):
    count = len(weights)
    rows, cols = weights[0].shape[1:]
    half = rows // lax.axis_size("grp")

    def kernel(gain_ref, *refs):
        sources, outs = refs[:count], refs[count : count + len(steps)]
        buf, sem = refs[count + len(steps) :]
        me, side = lax.axis_index("fs"), lax.axis_index("grp")
        span = aligned(side * half, half)
        copies = {}
        for n, k in enumerate(steps):
            for m in range(count):
                copies[n, m] = pltpu.make_async_copy(
                    sources[m].at[me ^ k, span], buf.at[n, m], sem.at[n, m]
                )
                copies[n, m].start()
        if scaled:
            factor = as_column(gain_ref[:, span], cols)
        for n in range(len(steps)):
            for m in range(count):
                copies[n, m].wait()
                value = buf[n, m]
                outs[n][m] = ((factor * value) if scaled else value).astype(BF16)

    shape = jax.ShapeDtypeStruct((count, half, cols), BF16)
    return pl.pallas_call(
        kernel,
        out_shape=(shape,) * len(steps),
        in_specs=[VMEM] + [ANY] * count,
        out_specs=(VMEM,) * len(steps),
        scratch_shapes=[
            pltpu.VMEM((len(steps), count, half, cols), F32),
            pltpu.SemaphoreType.DMA((len(steps), count)),
        ],
        name="cast_pieces",
    )(gain, *weights)


def assemble(out_refs, here, there, steps):
    me, side = lax.axis_index("fs"), lax.axis_index("grp")
    half = here[0].shape[1]
    for n, k in enumerate(steps):
        base = (me ^ k) * (2 * half)
        for m, out_ref in enumerate(out_refs):
            out_ref[aligned(base + side * half, half), :] = here[n][m]
            out_ref[aligned(base + (1 - side) * half, half), :] = there[n][m]


def ffn_block(quarters, gate_ref, up_ref):
    me = lax.axis_index("tp")
    width = quarters[0].shape[1]
    gate = up = None
    for k, rows_ref in enumerate(quarters):
        span = aligned((me ^ k) * width, width)
        rows = rows_ref[...]
        a = jnp.dot(rows, gate_ref[span, :], preferred_element_type=F32)
        b = jnp.dot(rows, up_ref[span, :], preferred_element_type=F32)
        gate = a if gate is None else gate + a
        up = b if up is None else up + b
    return (gate / (1.0 + jnp.exp(-gate)) * up).astype(BF16)


def ffn_first(gain, gate_weight, up_weight, here, there, steps, quarters):
    rows, cols = gate_weight.shape[1:]
    count = len(steps)
    chunk = quarters[0].shape[0]

    def kernel(gain_ref, gate_hbm, up_hbm, *refs):
        here_refs, there_refs = refs[:count], refs[count : 2 * count]
        x_refs = refs[2 * count : 2 * count + 4]
        gate_ref, up_ref, hidden_ref, buf, sem = refs[2 * count + 4 :]
        me = lax.axis_index("fs")
        copies = [
            pltpu.make_async_copy(source.at[me], buf.at[m], sem.at[m])
            for m, source in enumerate((gate_hbm, up_hbm))
        ]
        for copy in copies:
            copy.start()
        assemble((gate_ref, up_ref), here_refs, there_refs, steps)
        factor = as_column(gain_ref[...], cols)
        for m, out_ref in enumerate((gate_ref, up_ref)):
            copies[m].wait()
            out_ref[aligned(me * rows, rows), :] = (factor * buf[m]).astype(BF16)
        hidden_ref[...] = ffn_block(x_refs, gate_ref, up_ref)

    full = jax.ShapeDtypeStruct((rows * gate_weight.shape[0], cols), BF16)
    return pl.pallas_call(
        kernel,
        out_shape=(full, full, jax.ShapeDtypeStruct((chunk, cols), BF16)),
        in_specs=[VMEM, ANY, ANY] + [VMEM] * (2 * count + 4),
        out_specs=(VMEM, VMEM, VMEM),
        scratch_shapes=[pltpu.VMEM((2, rows, cols), F32), pltpu.SemaphoreType.DMA((2,))],
        name="ffn_first",
    )(gain, gate_weight, up_weight, *here, *there, *quarters)


def ffn_second(gate_out, up_out, quarters):
    def kernel(gate_ref, up_ref, *refs):
        refs[4][...] = ffn_block(refs[:4], gate_ref, up_ref)

    return pl.pallas_call(
        kernel,
        out_shape=jax.ShapeDtypeStruct((quarters[0].shape[0], gate_out.shape[1]), BF16),
        in_specs=[VMEM] * 6,
        out_specs=VMEM,
        name="ffn_second",
    )(gate_out, up_out, *quarters)


def join_down(down_weight, here, there, steps):
    rows, cols = down_weight.shape[1:]
    count = len(steps)
    total = rows * down_weight.shape[0]

    def kernel(down_hbm, *refs):
        out_ref, send_ref, buf, sem = refs[2 * count :]
        me = lax.axis_index("fs")
        copy = pltpu.make_async_copy(down_hbm.at[me], buf, sem)
        copy.start()
        assemble((out_ref,), refs[:count], refs[count : 2 * count], steps)
        copy.wait()
        out_ref[aligned(me * rows, rows), :] = buf[...].astype(BF16)
        other = 1 - lax.div(lax.axis_index("tp"), 2)
        send_ref[...] = out_ref[aligned(other * (total // 2), total // 2), :]

    return pl.pallas_call(
        kernel,
        out_shape=(
            jax.ShapeDtypeStruct((total, cols), BF16),
            jax.ShapeDtypeStruct((total // 2, cols), BF16),
        ),
        in_specs=[ANY] + [VMEM] * (2 * count),
        out_specs=(VMEM, VMEM),
        scratch_shapes=[pltpu.VMEM((rows, cols), F32), pltpu.SemaphoreType.DMA],
        name="join_down",
    )(down_weight, *here, *there)


def down_partial(hidden, hidden_x, down_out, down_x):
    chunk = hidden.shape[0]
    half = down_x.shape[0]
    quarter = half // 2

    def kernel(h_ref, hx_ref, down_ref, dx_ref, keep_ref, send_ref):
        me = lax.axis_index("tp")
        chip, core = lax.div(me, 2), lax.rem(me, 2)
        for out_ref, which in ((send_ref, 1 - core), (keep_ref, core)):
            a = down_ref[aligned(chip * half + which * quarter, quarter), :]
            b = dx_ref[aligned(which * quarter, quarter), :]
            dims = (((1,), (1,)), ((), ()))
            value = lax.dot_general(h_ref[...], a, dims, preferred_element_type=F32)
            value += lax.dot_general(hx_ref[...], b, dims, preferred_element_type=F32)
            out_ref[...] = value.astype(out_ref.dtype)

    return pl.pallas_call(
        kernel,
        out_shape=(
            jax.ShapeDtypeStruct((chunk, quarter), F32),
            jax.ShapeDtypeStruct((chunk, quarter), BF16),
        ),
        in_specs=[VMEM] * 4,
        out_specs=(VMEM, VMEM),
        name="down_partial",
    )(hidden, hidden_x, down_out, down_x)


def add_partials(keep, other):
    chunk, quarter = keep.shape

    def kernel(keep_ref, other_ref, a_ref, b_ref):
        total = (keep_ref[...] + other_ref[...].astype(F32)).astype(BF16)
        a_ref[...] = total[: chunk // 2]
        b_ref[...] = total[chunk // 2 :]

    shape = jax.ShapeDtypeStruct((chunk // 2, quarter), BF16)
    return pl.pallas_call(
        kernel, out_shape=(shape, shape), in_specs=[VMEM, VMEM], out_specs=(VMEM, VMEM),
        name="add_partials",
    )(keep, other)


def combine(ids_t, group_t, pair_t, rows, exp_group):
    n = ids_t.shape[1]
    capacity, width = rows[0].shape

    def kernel(ids_ref, group_ref, pair_ref, *refs):
        row_refs, out_ref = refs[:4], refs[4]
        ids = ids_ref[...]
        group, rank = group_ranks(ids, exp_group)
        group_exp = jnp.exp(group_ref[...])
        pair_exp = jnp.exp(pair_ref[...])
        lanes = lax.broadcasted_iota(jnp.int32, group_exp.shape, 0)
        chosen = jnp.sum(jnp.where(lanes == group, group_exp, 0.0), axis=0, keepdims=True)
        chosen = chosen / jnp.sum(group_exp, axis=0, keepdims=True)
        weight = pair_exp / jnp.sum(pair_exp, axis=0, keepdims=True) * chosen
        hit = lax.broadcasted_iota(jnp.int32, (capacity, n), 0) == rank
        me = lax.axis_index("fs")
        total = None
        for k in range(4):
            mine = jnp.sum(jnp.where(ids == (me ^ k), weight, 0.0), axis=0, keepdims=True)
            pick = jnp.where(hit, mine, 0.0).astype(BF16)
            part = lax.dot_general(
                pick, row_refs[k][...], (((0,), (0,)), ((), ())), preferred_element_type=F32
            )
            total = part if total is None else total + part
        out_ref[...] = total.astype(BF16)

    return pl.pallas_call(
        kernel,
        out_shape=jax.ShapeDtypeStruct((n, width), BF16),
        in_specs=[VMEM] * 7,
        out_specs=VMEM,
        name="combine",
    )(ids_t, group_t, pair_t, *rows)


def paired_body(
    tokens, norm_gain, gate_weight, up_weight, down_weight, expert_ids, group_logits, pair_logits
):
    experts = gate_weight.shape[0]
    capacity = 5 * tokens.shape[0] * 2 // (4 * experts)
    exp_group = experts // group_logits.shape[1]
    gain = norm_gain[None, :]
    ids_t = expert_ids.T
    steps = (3, 2, 1)

    gate_up = cast_pieces(gain, (gate_weight, up_weight), steps, True)
    own_rows, other_rows = gather_rows(ids_t, tokens, capacity, exp_group)
    cross = swap(other_rows, "fs", 2)
    gate_up_z = [swap(piece, "fs", k) for piece, k in zip(gate_up, steps)]
    pair = swap(own_rows, "fs", 1)
    cross_pair = swap(cross, "fs", 1)
    gate_up_y = [swap(piece, "grp", 1) for piece in gate_up_z]
    down = cast_pieces(gain, (down_weight,), steps, False)
    down_z = [swap(piece, "fs", k) for piece, k in zip(down, steps)]
    down_y = [swap(piece, "grp", 1) for piece in down_z]

    chunks = []
    for block in (
        jnp.concatenate([cross, cross_pair], axis=0),
        jnp.concatenate([own_rows, pair], axis=0),
    ):
        by_x = swap(block, "tp", 2)
        chunks.append((block, swap(block, "tp", 1), by_x, swap(by_x, "tp", 1)))
    gate_out, up_out, hidden_far = ffn_first(
        gain, gate_weight, up_weight, gate_up_z, gate_up_y, steps, chunks[0]
    )
    hidden_near = ffn_second(gate_out, up_out, chunks[1])
    down_out, down_send = join_down(down_weight, down_z, down_y, steps)
    down_x = swap(down_send, "tp", 2)
    done = []
    for hidden in (hidden_far, hidden_near):
        keep, send = down_partial(hidden, swap(hidden, "tp", 2), down_out, down_x)
        done += add_partials(keep, swap(send, "tp", 1))
    rows = (done[2], swap(done[3], "fs", 1), swap(done[0], "fs", 2), swap(done[1], "fs", 3))
    mixed = combine(ids_t, group_logits.T, pair_logits.T, rows, exp_group)
    return (mixed, gate_out[None], up_out[None], down_out[None])


def choose_body(*args):
    tokens, _, gate_weight, *_, group_logits, _ = args
    experts, rows, _ = gate_weight.shape
    paired = (
        lax.axis_size("grp") == 2
        and lax.axis_size("fs") == 4
        and lax.axis_size("tp") == 4
        and experts == 4
        and group_logits.shape[1] == 2
        and rows == tokens.shape[1]
    )
    return paired_body(*args) if paired else general_body(*args)


def solution(mesh):
    placed = (
        P(("grp", "fs"), "tp"),
        P("fs"),
        P(None, "fs", "tp"),
        P(None, "fs", "tp"),
        P(None, "fs", "tp"),
        P(("grp", "fs"), None),
        P(("grp", "fs"), None),
        P(("grp", "fs"), None),
    )
    return jax.shard_map(
        choose_body,
        mesh=mesh,
        in_specs=placed,
        out_specs=(
            P(("grp", "fs"), "tp"),
            P(("grp", "fs"), None, "tp"),
            P(("grp", "fs"), None, "tp"),
            P(("grp", "fs"), None, "tp"),
        ),
        check_vma=False,
    )
```
